32 devices in a mesh: grp: 2 (over y), tp: 4 (over z), dp: 4 (over x, core).
Axes of the slice: x: 2, y: 2, z: 4, core: 2. Of those that a mesh axis runs over, the one named last changes fastest.
Arguments:
- tokens: bfloat16 [128, 8, 2048], P('grp', None, 'dp'), parts along dimension 0, may hold values from -64 to 64
- live_counts: int32 [128], P(('grp', 'dp')), parts along dimension 0, may hold values from 1 to 8, 256 in all
- norm_gain: float32 [2, 2048], P(None, 'dp'), may hold values from 0.1 to 1.9
- w_branch: bfloat16 [2, 2048, 4096], P(None, 'dp', 'tp'), may hold values from -0.125 to 0.125
- w_silu_gate: bfloat16 [2, 2048, 4096], P(None, 'dp', 'tp'), may hold values from -0.125 to 0.125
- conv_weight: float32 [2, 4, 4096], P(None, None, 'tp'), may hold values from -3 to 3
- w_query: bfloat16 [2, 16, 256, 256], P(None, 'tp'), may hold values from -0.375 to 0.375
- w_key: bfloat16 [2, 16, 256, 256], P(None, 'tp'), may hold values from -0.375 to 0.375
- w_value: bfloat16 [2, 16, 256, 256], P(None, 'tp'), may hold values from -0.375 to 0.375
- w_input_gate: bfloat16 [2, 16, 768], P(None, 'tp'), may hold values from -0.21875 to 0.21875
- w_forget_gate: bfloat16 [2, 16, 768], P(None, 'tp'), may hold values from -0.21875 to 0.21875
- bias_input: float32 [2, 16], P(None, 'tp'), may hold values from -2 to 2
- bias_forget: float32 [2, 16], P(None, 'tp'), may hold values from -1 to 5
- out_gain: float32 [2, 16, 256], P(None, 'tp'), may hold values from 0.25 to 4
- skip_gain: float32 [2, 4096], P(None, 'tp'), may hold values from 0.25 to 4
- w_out: bfloat16 [2, 4096, 2048], P(None, 'tp', 'dp'), may hold values from -0.09375 to 0.09375
- conv_state: bfloat16 [2, 128, 3, 4096], P(None, ('grp', 'dp'), None, 'tp'), parts along dimension 1, may hold values from -6 to 6
- memory: float32 [2, 128, 16, 256, 256], P(None, ('grp', 'dp'), 'tp'), parts along dimension 1, may hold values from -0.375 to 0.375
- max_state: float32 [2, 128, 16], P(None, ('grp', 'dp'), 'tp'), parts along dimension 1, may hold values from -4 to 4
Outputs:
- out_tokens: bfloat16 [128, 8, 2048], P('grp', None, 'dp'), parts along dimension 0
- new_conv_state: bfloat16 [2, 128, 3, 4096], P(None, ('grp', 'dp'), None, 'tp'), parts along dimension 1
- new_memory: float32 [2, 128, 16, 256, 256], P(None, ('grp', 'dp'), 'tp'), parts along dimension 1
- new_max: float32 [2, 128, 16], P(None, ('grp', 'dp'), 'tp'), parts along dimension 1
The draws below stay inside these ranges and needn't reach their ends.
There are 2 independent parts, one for each index of `grp`. The reference program is written for one: setup_inputs(seed, part) draws one part's arguments, and reference() takes and returns one part's arrays. A program takes and returns all parts, laid end to end along the dimension named above; an argument that names none is the same for every part. Nothing has to cross between parts.
Inputs may be any that keep to these rules, and one draw needn't show every extreme that they name: `live_counts`: each sequence has at least one live slot; within each part (each independent copy of the problem) the 64 counts sum to 256, so the whole array sums to that times the number of parts; in each part some sequence uses all 8 slots.
All inputs are finite; a program needn't handle non-finite values. No bound on the sum of `live_counts` on one device may be relied on, other than what follows from the above.
Results may differ from the reference program's by a relative error of at most 0.035.
Values may be sent and summed in bfloat16 or wider, within the bound.
A program may use at most 192 MiB of HBM per device.

```python
import math
import jax
import jax.numpy as jnp
import numpy as np
from jax import lax

D = 2048
HEADS = 16
HEAD_DIM = 256
CONV = 4
LAYERS = 2
NEW = 8
BATCH = 64
INNER = 4096
N_DP = 4


def draw_tokens(key, part):
    first_key, second_key = jax.random.split(jax.random.fold_in(key, 11), 2)
    features = jnp.arange(D, dtype=jnp.float32) / D
    column_scale = jnp.exp(jnp.log(6.0) * features + jax.random.uniform(second_key, (D,), jnp.float32, -0.4, 0.4))
    base = jnp.clip(jax.random.normal(first_key, (BATCH, NEW, D), jnp.float32), -4.0, 4.0)
    return (base * column_scale).astype(jnp.bfloat16)


def block_scale(own_key, dims, pieces, low, largest):
    level, own = 1.0, jax.random.fold_in(own_key, 6)
    for position, shards_of in pieces:
        steps = jnp.exp(jax.random.uniform(jax.random.fold_in(own, position), (shards_of,), jnp.float32, low / len(pieces), largest / len(pieces)))
        level = level * jnp.repeat(steps, dims[position] // shards_of).reshape([-1 if axis == position else 1 for axis in range(len(dims))])
    return level


def length_profile(count, total, bound, lean):
    weights = [(1 << 20) // math.isqrt(standing ** lean) + 1 for standing in range(2, count + 1)]
    surplus, holding = total - bound - (count - 1), [1] * (count - 1)
    while surplus > 0:
        movable = [i for i in range(count - 1) if holding[i] < bound]
        pool, budget = sum([weights[i] for i in movable]), surplus
        for i in movable:
            extra = min(bound - holding[i], max(1, budget * weights[i] // pool), surplus)
            holding[i] = holding[i] + extra
            surplus = surplus - extra
    return np.array([bound] + holding)


def uneven(key, number_of, total, bound, slope):
    if number_of == 2:
        one = jax.random.randint(key, (), max(1, total - bound), min(bound, total - 1) + 1)
        return jnp.stack([one, total - one])
    tallies = jnp.asarray(length_profile(number_of, total, bound, slope), jnp.int32)
    pairs = (number_of - 1) // 2
    donor, receiver = tallies[1:1 + 2 * pairs:2], tallies[2:2 + 2 * pairs:2]
    margin = jnp.minimum(donor - 1, bound - receiver)
    shifted = jax.random.randint(jax.random.fold_in(key, 1), (pairs,), 0, 1 << 20) % (margin + 1)
    tallies = tallies.at[1:1 + 2 * pairs:2].set(donor - shifted).at[2:2 + 2 * pairs:2].set(receiver + shifted)
    return tallies[jax.random.permutation(jax.random.fold_in(key, 2), number_of)]


def normal_values(rng, dims, deviation, most, cuts=(), kind=jnp.bfloat16):
    level = block_scale(rng, dims, cuts, -0.22, 0.18) if cuts else 1.0
    entries = jax.random.normal(rng, dims, jnp.float32) * deviation * level
    return jnp.minimum(jnp.maximum(entries, -most), most).astype(kind)


def setup_inputs(seed: int = 0, part: int = 0) -> dict:
    keys = jax.random.split(jax.random.key(seed), 20)
    part_keys = jax.random.split(jax.random.fold_in(keys[19], part), 20)
    return {
        "tokens": draw_tokens(jax.random.fold_in(jax.random.fold_in(keys[19], part), 71), part),
        "live_counts": uneven(part_keys[1], BATCH, BATCH * NEW // 2, NEW, 2).astype(jnp.int32),
        "norm_gain": jnp.clip(1.0 + 0.18 * jax.random.normal(keys[2], (LAYERS, D), jnp.float32), 0.1, 1.9),
        "w_branch": normal_values(keys[3], (LAYERS, D, INNER), D ** -0.5, 0.125, ((1, 4), (2, 4))),
        "w_silu_gate": normal_values(keys[4], (LAYERS, D, INNER), D ** -0.5, 0.125, ((1, 4), (2, 4))),
        "conv_weight": normal_values(keys[5], (LAYERS, CONV, INNER), CONV ** -0.5, 3.0, ((2, 4),), jnp.float32),
        "w_query": normal_values(keys[6], (LAYERS, HEADS, HEAD_DIM, HEAD_DIM), HEAD_DIM ** -0.5, 0.375, ((1, 4),)),
        "w_key": normal_values(keys[7], (LAYERS, HEADS, HEAD_DIM, HEAD_DIM), HEAD_DIM ** -0.5, 0.375, ((1, 4),)),
        "w_value": normal_values(keys[8], (LAYERS, HEADS, HEAD_DIM, HEAD_DIM), HEAD_DIM ** -0.5, 0.375, ((1, 4),)),
        "w_input_gate": normal_values(keys[9], (LAYERS, HEADS, 3 * HEAD_DIM), (3 * HEAD_DIM) ** -0.5, 0.21875, ((1, 4),)),
        "w_forget_gate": normal_values(keys[10], (LAYERS, HEADS, 3 * HEAD_DIM), (3 * HEAD_DIM) ** -0.5, 0.21875, ((1, 4),)),
        "bias_input": jnp.clip(jax.random.uniform(keys[11], (LAYERS, HEADS), jnp.float32, -2.0, 2.0) * block_scale(keys[11], (LAYERS, HEADS), ((1, 4),), -0.4, 0.0), -2.0, 2.0),
        "bias_forget": jnp.clip(-1.0 + 6.0 * jax.random.uniform(keys[12], (LAYERS, HEADS), jnp.float32) ** block_scale(keys[12], (LAYERS, HEADS), ((1, 4),), -0.2, 0.2), -1.0, 5.0),
        "out_gain": jnp.clip(jnp.exp(math.log(4.0) - 2.7725887 * jax.random.uniform(keys[13], (LAYERS, HEADS, HEAD_DIM), jnp.float32) ** block_scale(keys[13], (LAYERS, HEADS, HEAD_DIM), ((1, 4),), -0.2, 0.2)), 0.25, 4.0),
        "skip_gain": jnp.clip(jnp.exp(math.log(4.0) - 2.7725887 * jax.random.uniform(keys[14], (LAYERS, INNER), jnp.float32) ** block_scale(keys[14], (LAYERS, INNER), ((1, 4),), -0.2, 0.2)), 0.25, 4.0),
        "w_out": normal_values(keys[15], (LAYERS, INNER, D), INNER ** -0.5, 0.09375, ((1, 4), (2, 4))),
        "conv_state": normal_values(part_keys[16], (LAYERS, BATCH, CONV - 1, INNER), 1.0, 6.0, ((1, 4), (3, 4))),
        "memory": normal_values(part_keys[17], (LAYERS, BATCH, HEADS, HEAD_DIM, HEAD_DIM), (HEAD_DIM ** -0.5), 0.375, ((1, 4), (2, 4)), jnp.float32),
        "max_state": normal_values(part_keys[18], (LAYERS, BATCH, HEADS), 1.0, 4.0, ((1, 4), (2, 4)), jnp.float32),
    }


epsilon = 1e-06
very_negative = -1e+30

def layer_step(tokens, live_counts, gain, w_branch, w_silu_gate, conv_weight, w_query, w_key, w_value, w_input_gate, w_forget_gate, bias_input, bias_forget, out_gain, skip_gain, w_out, conv_state, memory, max_state):
    floats = tokens.astype(jnp.float32)
    mean_square = lax.optimization_barrier(jnp.mean(floats * floats, axis=-1, keepdims=True))
    normed = (floats * lax.rsqrt(mean_square + epsilon) * gain).astype(jnp.bfloat16)
    flat = normed.reshape(BATCH * NEW, D)
    block_rows = D // N_DP
    branch_sum = jnp.zeros((BATCH * NEW, INNER), jnp.float32)
    gate_sum = jnp.zeros((BATCH * NEW, INNER), jnp.float32)
    for block in range(N_DP):
        lower = block * block_rows
        rows = flat[:, lower:lower + block_rows]
        first = jnp.dot(rows, w_branch[lower:lower + block_rows], preferred_element_type=jnp.float32)
        second = jnp.dot(rows, w_silu_gate[lower:lower + block_rows], preferred_element_type=jnp.float32)
        branch_sum = branch_sum + first.astype(jnp.bfloat16).astype(jnp.float32)
        gate_sum = gate_sum + second.astype(jnp.bfloat16).astype(jnp.float32)
    branch = branch_sum.astype(jnp.bfloat16).reshape(BATCH, NEW, INNER)
    silu_gate = gate_sum.astype(jnp.bfloat16).reshape(BATCH, NEW, INNER)
    padded = jnp.concatenate([conv_state, branch], axis=1)
    conv_sum = jnp.zeros((BATCH, NEW, INNER), jnp.float32)
    for offset in range(CONV):
        conv_sum = conv_sum + padded[:, offset:offset + NEW].astype(jnp.float32) * conv_weight[offset]
    convolved = jax.nn.silu(conv_sum).astype(jnp.bfloat16)
    picks = live_counts[:, None] + jnp.arange(CONV - 1, dtype=jnp.int32)[None, :]
    new_conv = jnp.take_along_axis(padded, picks[:, :, None], axis=1)
    conv_heads = convolved.reshape(BATCH, NEW, HEADS, HEAD_DIM).astype(jnp.float32)
    branch_heads = branch.reshape(BATCH, NEW, HEADS, HEAD_DIM).astype(jnp.float32)
    queries = jnp.einsum('blhd,hde->blhe', conv_heads, w_query.astype(jnp.float32)).astype(jnp.bfloat16)
    key_rows = jnp.einsum('blhd,hde->blhe', conv_heads, w_key.astype(jnp.float32)).astype(jnp.bfloat16)
    value_rows = jnp.einsum('blhd,hde->blhe', branch_heads, w_value.astype(jnp.float32)).astype(jnp.bfloat16)
    joined = jnp.concatenate([queries, key_rows, value_rows], axis=-1).astype(jnp.float32)
    input_log = jnp.einsum('blhc,hc->blh', joined, w_input_gate.astype(jnp.float32)) + bias_input
    forget_log = jax.nn.log_sigmoid(jnp.einsum('blhc,hc->blh', joined, w_forget_gate.astype(jnp.float32)) + bias_forget)
    positions = jnp.arange(NEW, dtype=jnp.int32)
    live = positions[None, :] < live_counts[:, None]
    input_log = jnp.transpose(jnp.where(live[:, :, None], input_log, very_negative), (0, 2, 1))
    forget_log = jnp.transpose(jnp.where(live[:, :, None], forget_log, 0.0), (0, 2, 1))
    query_heads = jnp.transpose(queries.astype(jnp.float32), (0, 2, 1, 3))
    key_heads = jnp.transpose(key_rows.astype(jnp.float32), (0, 2, 1, 3)) * HEAD_DIM ** (-0.5)
    value_heads = jnp.transpose(value_rows.astype(jnp.float32), (0, 2, 1, 3))
    cumulative = jnp.cumsum(forget_log, axis=-1)
    log_weights = cumulative[..., :, None] - cumulative[..., None, :] + input_log[..., None, :]
    causal = positions[:, None] >= positions[None, :]
    log_weights = jnp.where(causal, log_weights, very_negative)
    carried = cumulative + max_state[..., None]
    stabilizer = jnp.maximum(lax.optimization_barrier(jnp.max(log_weights, axis=-1)), carried)
    weights = jnp.exp(log_weights - stabilizer[..., None])
    carried_scale = jnp.exp(carried - stabilizer)
    scores = jnp.einsum('bhtd,bhsd->bhts', query_heads, key_heads) * weights
    numerator = jnp.einsum('bhts,bhse->bhte', scores, value_heads)
    numerator = numerator + carried_scale[..., None] * jnp.einsum('bhtd,bhde->bhte', query_heads, memory)
    centered = numerator - lax.optimization_barrier(jnp.mean(numerator, axis=-1, keepdims=True))
    normalized = centered * lax.rsqrt(lax.optimization_barrier(jnp.mean(centered * centered, axis=-1, keepdims=True)) + epsilon)
    normalized = normalized * out_gain[None, :, None, :]
    readout = jnp.transpose(normalized, (0, 2, 1, 3)).reshape(BATCH, NEW, INNER)
    new_max = stabilizer[..., -1]
    decay = jnp.exp(cumulative[..., -1] + max_state - new_max)
    update_weight = jnp.exp(cumulative[..., -1:] - cumulative + input_log - new_max[..., None])
    new_memory = decay[..., None, None] * memory + jnp.einsum('bhs,bhsd,bhse->bhde', update_weight, key_heads, value_heads)
    mixed = (readout + skip_gain * convolved.astype(jnp.float32)) * jax.nn.silu(silu_gate.astype(jnp.float32))
    mixed = jnp.where(live[:, :, None], mixed, 0.0).astype(jnp.bfloat16)
    projected = jnp.dot(mixed.reshape(BATCH * NEW, INNER), w_out, preferred_element_type=jnp.float32)
    projected = projected.astype(jnp.bfloat16).reshape(BATCH, NEW, D)
    result = (floats + projected.astype(jnp.float32)).astype(jnp.bfloat16)
    return (result, new_conv, new_memory, new_max)

def reference(tokens, live_counts, norm_gain, w_branch, w_silu_gate, conv_weight, w_query, w_key, w_value, w_input_gate, w_forget_gate, bias_input, bias_forget, out_gain, skip_gain, w_out, conv_state, memory, max_state):
    stream = tokens
    conv_list = []
    memory_list = []
    max_list = []
    for which_layer in range(LAYERS):
        stream, new_conv, new_memory, new_max = layer_step(stream, live_counts, norm_gain[which_layer], w_branch[which_layer], w_silu_gate[which_layer], conv_weight[which_layer], w_query[which_layer], w_key[which_layer], w_value[which_layer], w_input_gate[which_layer], w_forget_gate[which_layer], bias_input[which_layer], bias_forget[which_layer], out_gain[which_layer], skip_gain[which_layer], w_out[which_layer], conv_state[which_layer], memory[which_layer], max_state[which_layer])
        conv_list.append(new_conv)
        memory_list.append(new_memory)
        max_list.append(new_max)
    return (stream, jnp.stack(conv_list), jnp.stack(memory_list), jnp.stack(max_list))
```

```python
import functools

import jax
import jax.numpy as jnp
from jax import lax
from jax.experimental import pallas as pl
from jax.experimental.pallas import tpu as pltpu
from jax.sharding import PartitionSpec as P

HEAD_DIM = 256
CONV = 4
LAYERS = 2
epsilon = 1e-06
very_negative = -1e30

VM = pl.BlockSpec(memory_space=pltpu.VMEM)
MESH = pl.DeviceIdType.MESH


def greet(axis, devices):
    barrier = pltpu.get_barrier_semaphore()
    for device in devices:
        pl.semaphore_signal(barrier, inc=1, device_id={axis: device}, device_id_type=MESH)
    pl.semaphore_wait(barrier, len(devices))


def rcopy(src, dst, send, recv, axis, device):
    return pltpu.make_async_remote_copy(
        src_ref=src, dst_ref=dst, send_sem=send, recv_sem=recv,
        device_id={axis: device}, device_id_type=MESH,
    )


def scatter_kernel(n, chunks, a_ref, b_ref, aux_ref, oa_ref, ob_ref, oaux_ref,
                   r1a, r1b, s2a, s2b, r2a, r2b, s1s, s1r, s2s, s2r, axs, axr):
    nx = n // 2
    me = lax.axis_index("dp")
    core = me % 2
    x = me // 2
    partner = me + 1 - 2 * core
    greet("dp", [(me + off) % n for off in range(1, n)])
    started = []
    aux_copies = []
    first = {}
    for g in range(nx):
        xo = (x + 1 + g) % nx
        for c in range(chunks):
            pair = []
            for k, (src, dst) in enumerate(((a_ref, r1a), (b_ref, r1b))):
                cp = rcopy(src.at[xo, 1 - core, c], dst.at[g, c],
                           s1s.at[g, c, k], s1r.at[g, c, k], "dp", partner)
                cp.start()
                pair.append(cp)
                started.append(cp)
            first[g, c] = pair
        if g == 0:
            for off in range(1, n):
                to = (me + off) % n
                cp = rcopy(aux_ref.at[to], oaux_ref.at[me], axs.at[off - 1], axr.at[off - 1], "dp", to)
                cp.start()
                aux_copies.append(cp)
                started.append(cp)
            oaux_ref[me] = aux_ref[me]
    second = {}
    for g in range(nx - 1):
        xo = (x + 1 + g) % nx
        for c in range(chunks):
            pair = []
            for k, (src, got, buf, dst) in enumerate(((a_ref, r1a, s2a, r2a), (b_ref, r1b, s2b, r2b))):
                first[g, c][k].wait_recv()
                buf[g, c] = (
                    src[xo, core, c].astype(jnp.float32) + got[g, c].astype(jnp.float32)
                ).astype(jnp.bfloat16)
                cp = rcopy(buf.at[g, c], dst.at[g, c], s2s.at[g, c, k], s2r.at[g, c, k],
                           "dp", 2 * xo + core)
                cp.start()
                pair.append(cp)
                started.append(cp)
            second[g, c] = pair
    for c in range(chunks):
        for k, (src, got, more, out) in enumerate(((a_ref, r1a, r2a, oa_ref), (b_ref, r1b, r2b, ob_ref))):
            first[nx - 1, c][k].wait_recv()
            total = src[x, core, c].astype(jnp.float32) + got[nx - 1, c].astype(jnp.float32)
            for g in range(nx - 1):
                second[g, c][k].wait_recv()
                total = total + more[g, c].astype(jnp.float32)
            out[c] = total
    for cp in aux_copies:
        cp.wait_recv()
    for cp in started:
        cp.wait_send()


def scatter_dp(n, a, b, aux):
    rows, width = a.shape
    nx = n // 2
    own = rows // n
    chunks = 4 if own % 64 == 0 else 1
    piece = own // chunks
    a = a.reshape(nx, 2, chunks, piece, width)
    b = b.reshape(nx, 2, chunks, piece, width)
    far = max(nx - 1, 1)
    bf = jnp.bfloat16
    sem = pltpu.SemaphoreType.DMA
    oa, ob, oaux = pl.pallas_call(
        functools.partial(scatter_kernel, n, chunks),
        out_shape=(
            jax.ShapeDtypeStruct((chunks, piece, width), jnp.float32),
            jax.ShapeDtypeStruct((chunks, piece, width), jnp.float32),
            jax.ShapeDtypeStruct(aux.shape, jnp.float32),
        ),
        in_specs=[VM] * 3,
        out_specs=(VM,) * 3,
        scratch_shapes=[
            pltpu.VMEM((nx, chunks, piece, width), bf),
            pltpu.VMEM((nx, chunks, piece, width), bf),
            pltpu.VMEM((far, chunks, piece, width), bf),
            pltpu.VMEM((far, chunks, piece, width), bf),
            pltpu.VMEM((far, chunks, piece, width), bf),
            pltpu.VMEM((far, chunks, piece, width), bf),
            sem((nx, chunks, 2)), sem((nx, chunks, 2)),
            sem((far, chunks, 2)), sem((far, chunks, 2)),
            sem((n - 1,)), sem((n - 1,)),
        ],
        compiler_params=pltpu.CompilerParams(collective_id=0, has_side_effects=True),
        name="scatter_dp",
    )(a, b, aux)
    return oa.reshape(own, width), ob.reshape(own, width), oaux


def gather_kernel(n, chunks, m_ref, out_ref, xs, xr, ps, pr, fs, fr):
    nx = n // 2
    me = lax.axis_index("dp")
    core = me % 2
    x = me // 2
    partner = me + 1 - 2 * core
    greet("dp", [partner] + [2 * ((x + 1 + g) % nx) + core for g in range(nx - 1)])
    started = []
    across = {}
    near = {}
    for c in range(chunks):
        for g in range(nx - 1):
            to = 2 * ((x + 1 + g) % nx) + core
            cp = rcopy(m_ref.at[c], out_ref.at[x, core, c], xs.at[g, c], xr.at[g, c], "dp", to)
            cp.start()
            across[g, c] = cp
            started.append(cp)
    for c in range(chunks):
        cp = rcopy(m_ref.at[c], out_ref.at[x, core, c], ps.at[c], pr.at[c], "dp", partner)
        cp.start()
        near[c] = cp
        started.append(cp)
    out_ref[x, core] = m_ref[...]
    passed = []
    for c in range(chunks):
        for g in range(nx - 1):
            origin = (x + nx - 1 - g) % nx
            across[g, c].wait_recv()
            cp = rcopy(out_ref.at[origin, core, c], out_ref.at[origin, core, c],
                       fs.at[g, c], fr.at[g, c], "dp", partner)
            cp.start()
            passed.append(cp)
            started.append(cp)
    for c in range(chunks):
        near[c].wait_recv()
    for cp in passed:
        cp.wait_recv()
    for cp in started:
        cp.wait_send()


def gather_dp(n, m):
    own, width = m.shape
    nx = n // 2
    chunks = 4 if own % 64 == 0 else 1
    piece = own // chunks
    far = max(nx - 1, 1)
    sem = pltpu.SemaphoreType.DMA
    out = pl.pallas_call(
        functools.partial(gather_kernel, n, chunks),
        out_shape=jax.ShapeDtypeStruct((nx, 2, chunks, piece, width), m.dtype),
        in_specs=[VM],
        out_specs=VM,
        scratch_shapes=[
            sem((far, chunks)), sem((far, chunks)), sem((chunks,)), sem((chunks,)),
            sem((far, chunks)), sem((far, chunks)),
        ],
        compiler_params=pltpu.CompilerParams(collective_id=1, has_side_effects=True),
        name="gather_dp",
    )(m.reshape(chunks, piece, width))
    return out.reshape(n * own, width)


def reduce_kernel(n, p_ref, x_ref, out_ref, got, mine, s1, r1, s2, r2):
    me = lax.axis_index("tp")
    greet("tp", [(me + off) % n for off in range(1, n)])
    started = []
    first = []
    order = sorted(range(1, n), key=lambda off: -min(off, n - off))
    for off in order:
        to = (me + off) % n
        cp = rcopy(p_ref.at[to], got.at[off - 1], s1.at[off - 1], r1.at[off - 1], "tp", to)
        cp.start()
        started.append(cp)
        first.append((off, cp))
    total = p_ref[me].astype(jnp.float32)
    for off, cp in first:
        cp.wait_recv()
        total = total + got[off - 1].astype(jnp.float32)
    update = total.astype(jnp.bfloat16).astype(jnp.float32)
    mine[...] = (x_ref[me].astype(jnp.float32) + update).astype(jnp.bfloat16)
    second = []
    for off in order:
        to = (me + off) % n
        cp = rcopy(mine, out_ref.at[me], s2.at[off - 1], r2.at[off - 1], "tp", to)
        cp.start()
        started.append(cp)
        second.append(cp)
    out_ref[me] = mine[...]
    for cp in second:
        cp.wait_recv()
    for cp in started:
        cp.wait_send()


def reduce_tp(n, p, x):
    rows, width = p.shape
    share = rows // n
    sem = pltpu.SemaphoreType.DMA
    out = pl.pallas_call(
        functools.partial(reduce_kernel, n),
        out_shape=jax.ShapeDtypeStruct((n, share, width), jnp.bfloat16),
        in_specs=[VM] * 2,
        out_specs=VM,
        scratch_shapes=[
            pltpu.VMEM((n - 1, share, width), jnp.bfloat16),
            pltpu.VMEM((share, width), jnp.bfloat16),
            sem((n - 1,)), sem((n - 1,)), sem((n - 1,)), sem((n - 1,)),
        ],
        compiler_params=pltpu.CompilerParams(collective_id=2, has_side_effects=True),
        name="reduce_tp",
    )(p.reshape(n, share, width), x.reshape(n, share, width))
    return out.reshape(rows, width)


def cell_kernel(heads, q_ref, k_ref, v_ref, w_ref, s_ref, c_ref, *rest):
    num_ref, new_ref = rest[-2:]
    for h in range(heads):
        q = q_ref[0, h]
        k = k_ref[0, h]
        v = v_ref[0, h]
        scal = s_ref[0, h]
        old = c_ref[0, 0, h]
        scores = lax.dot_general(q, k, (((1,), (1,)), ((), ())), preferred_element_type=jnp.float32)
        scores = scores * w_ref[0, h]
        inside = jnp.dot(scores, v, preferred_element_type=jnp.float32)
        carried = jnp.dot(
            q.astype(jnp.bfloat16), old.astype(jnp.bfloat16), preferred_element_type=jnp.float32
        )
        num_ref[0, h] = inside + scal[:, 0:1] * carried
        outer = lax.dot_general(
            k * scal[:, 1:2], v, (((0,), (0,)), ((), ())), preferred_element_type=jnp.float32
        )
        new_ref[0, 0, h] = scal[0:1, 2:3] * old + outer


def memory_cell(layer, q, k, v, weights, scal, memory, previous):
    batch, heads, steps, dim = q.shape
    row = pl.BlockSpec((1, heads, steps, dim), lambda b: (b, 0, 0, 0))
    small = pl.BlockSpec((1, heads, steps, steps), lambda b: (b, 0, 0, 0))
    three = pl.BlockSpec((1, heads, steps, 3), lambda b: (b, 0, 0, 0))
    mat = pl.BlockSpec((1, 1, heads, dim, dim), lambda b: (layer, b, 0, 0, 0))
    args = [q, k, v, weights, scal, memory]
    specs = [row, row, row, small, three, mat]
    aliases = {}
    if previous is not None:
        args.append(previous)
        specs.append(pl.BlockSpec(memory_space=pl.ANY))
        aliases = {6: 1}
    return pl.pallas_call(
        functools.partial(cell_kernel, heads),
        grid=(batch,),
        out_shape=(
            jax.ShapeDtypeStruct(q.shape, jnp.float32),
            jax.ShapeDtypeStruct(memory.shape, jnp.float32),
        ),
        in_specs=specs,
        out_specs=(row, mat),
        input_output_aliases=aliases,
        compiler_params=pltpu.CompilerParams(dimension_semantics=("arbitrary",)),
        name="memory_cell",
    )(*args)


def per_device(tokens, live_counts, norm_gain, w_branch, w_silu_gate, conv_weight, w_query, w_key,
               w_value, w_input_gate, w_forget_gate, bias_input, bias_forget, out_gain, skip_gain,
               w_out, conv_state, memory, max_state):
    f32 = jnp.float32
    bf = jnp.bfloat16
    ndp = lax.axis_size("dp")
    ntp = lax.axis_size("tp")
    all_batch, steps, features = tokens.shape
    batch = live_counts.shape[0]
    width = w_branch.shape[2]
    heads = w_query.shape[1]
    rows = all_batch * steps
    own = batch * steps
    live_rows = all_batch * steps // 2
    lanes = -(-own // 128) * 128
    model = features * ndp
    flat_tokens = tokens.reshape(rows, features)
    positions = jnp.arange(steps, dtype=jnp.int32)
    live = positions[None, :] < live_counts[:, None]
    causal = positions[:, None] >= positions[None, :]
    picks = live_counts[:, None] + jnp.arange(CONV - 1, dtype=jnp.int32)[None, :]
    pick_hot = picks[:, :, None] == jnp.arange(steps + CONV - 1, dtype=jnp.int32)[None, None, :]
    count_row = jnp.pad(live_counts.astype(f32), (0, lanes - batch))

    dense = flat_tokens
    compact = None
    select = None
    live_all = None
    new_memory = None
    conv_list = []
    max_list = []
    for l in range(LAYERS):
        floats = dense.astype(f32)
        squares = jnp.sum(floats * floats, axis=-1).reshape(ndp, own)
        squares = jnp.pad(squares, ((0, 0), (0, lanes - own)))
        aux = jnp.stack([squares, jnp.broadcast_to(count_row, squares.shape)], axis=1)
        aux = jnp.pad(aux, ((0, 0), (0, 6), (0, 0)))
        scaled = (floats * norm_gain[l]).astype(bf)
        first = jnp.dot(scaled, w_branch[l], preferred_element_type=f32).astype(bf)
        second = jnp.dot(scaled, w_silu_gate[l], preferred_element_type=f32).astype(bf)
        branch, gate, aux = scatter_dp(ndp, first, second, aux)
        total = jnp.sum(aux[:, 0, :own], axis=0)
        inv = lax.rsqrt(total / model + epsilon)[:, None]
        branch = (branch * inv).astype(bf).reshape(batch, steps, width)
        gate = (gate * inv).astype(bf).astype(f32).reshape(batch, steps, width)
        if select is None:
            counts = aux[:, 1, :batch].astype(jnp.int32).reshape(all_batch)
            ids = jnp.arange(all_batch)
            before = jnp.sum(jnp.where(ids[None, :] < ids[:, None], counts[None, :], 0), axis=1)
            live_all = positions[None, :] < counts[:, None]
            place = jnp.where(live_all, before[:, None] + positions[None, :], -1).reshape(rows)
            select = (jnp.arange(live_rows)[:, None] == place[None, :]).astype(bf)
            compact = jnp.dot(select, flat_tokens, preferred_element_type=f32).astype(bf)

        padded = jnp.concatenate([conv_state[l], branch], axis=1).astype(f32)
        conv_sum = padded[:, 0:steps] * conv_weight[l, 0]
        for j in range(1, CONV):
            conv_sum = conv_sum + padded[:, j:j + steps] * conv_weight[l, j]
        convolved = jax.nn.silu(conv_sum).astype(bf)
        new_conv = jnp.stack(
            [jnp.sum(jnp.where(pick_hot[:, i, :, None], padded, 0.0), axis=1) for i in range(CONV - 1)],
            axis=1,
        ).astype(bf)
        conv_list.append(new_conv)
        conv_flat = convolved.reshape(own, width)
        branch_flat = branch.reshape(own, width)

        def project(source, w):
            parts = [
                jnp.dot(source[:, h * HEAD_DIM:(h + 1) * HEAD_DIM], w[h], preferred_element_type=f32)
                for h in range(heads)
            ]
            out = jnp.stack([p.reshape(batch, steps, HEAD_DIM) for p in parts], axis=1)
            return out.astype(bf).astype(f32)

        q = project(conv_flat, w_query[l])
        k = project(conv_flat, w_key[l])
        v = project(branch_flat, w_value[l])

        def gate_dot(w, bias):
            w = w.astype(f32).reshape(heads, 3, 1, HEAD_DIM)
            return jnp.sum(q * w[:, 0] + k * w[:, 1] + v * w[:, 2], axis=-1) + bias[:, None]

        live_h = live[:, None, :]
        ig = jnp.where(live_h, gate_dot(w_input_gate[l], bias_input[l]), very_negative)
        fg = jnp.where(live_h, jax.nn.log_sigmoid(gate_dot(w_forget_gate[l], bias_forget[l])), 0.0)
        cum = jnp.sum(jnp.where(causal, fg[..., None, :], 0.0), axis=-1)
        logw = cum[..., :, None] - cum[..., None, :] + ig[..., None, :]
        logw = jnp.where(causal, logw, very_negative)
        carried = cum + max_state[l][..., None]
        stab = jnp.maximum(jnp.max(logw, axis=-1), carried)
        weights = jnp.exp(logw - stab[..., None])
        new_max = stab[..., -1]
        decay = jnp.exp(cum[..., -1] + max_state[l] - new_max)
        upd = jnp.exp(cum[..., -1:] - cum + ig - new_max[..., None])
        scal = jnp.stack(
            [jnp.exp(carried - stab), upd, jnp.broadcast_to(decay[..., None], upd.shape)], axis=-1
        )
        max_list.append(new_max)
        num, new_memory = memory_cell(
            l, q, k * HEAD_DIM ** (-0.5), v, weights, scal, memory, new_memory
        )
        centered = num - jnp.mean(num, axis=-1, keepdims=True)
        normalized = centered * lax.rsqrt(
            jnp.mean(centered * centered, axis=-1, keepdims=True) + epsilon
        )
        normalized = normalized * out_gain[l][None, :, None, :]
        readout = jnp.transpose(normalized, (0, 2, 1, 3)).reshape(batch, steps, width)
        mixed = (readout + skip_gain[l] * convolved.astype(f32)) * jax.nn.silu(gate)
        mixed = jnp.where(live[:, :, None], mixed, 0.0).astype(bf).reshape(own, width)
        everyone = gather_dp(ndp, mixed)
        packed = jnp.dot(select, everyone, preferred_element_type=f32).astype(bf)
        part = jnp.dot(packed, w_out[l], preferred_element_type=f32).astype(bf)
        compact = reduce_tp(ntp, part, compact)
        dense = lax.dot_general(
            select, compact, (((0,), (0,)), ((), ())), preferred_element_type=f32
        ).astype(bf)
    result = jnp.where(live_all[:, :, None], dense.reshape(tokens.shape), tokens)
    return (result, jnp.stack(conv_list), new_memory, jnp.stack(max_list))


def solution(mesh):
    in_specs = (
        P("grp", None, "dp"),
        P(("grp", "dp")),
        P(None, "dp"),
        P(None, "dp", "tp"),
        P(None, "dp", "tp"),
        P(None, None, "tp"),
        P(None, "tp", None, None),
        P(None, "tp", None, None),
        P(None, "tp", None, None),
        P(None, "tp", None),
        P(None, "tp", None),
        P(None, "tp"),
        P(None, "tp"),
        P(None, "tp", None),
        P(None, "tp"),
        P(None, "tp", "dp"),
        P(None, ("grp", "dp"), None, "tp"),
        P(None, ("grp", "dp"), "tp", None, None),
        P(None, ("grp", "dp"), "tp"),
    )
    out_specs = (
        P("grp", None, "dp"),
        P(None, ("grp", "dp"), None, "tp"),
        P(None, ("grp", "dp"), "tp", None, None),
        P(None, ("grp", "dp"), "tp"),
    )
    return jax.shard_map(
        per_device, mesh=mesh, in_specs=in_specs, out_specs=out_specs, check_vma=False
    )
```

```python
import functools

import jax
import jax.numpy as jnp
from jax import lax
from jax.experimental import pallas as pl
from jax.experimental.pallas import tpu as pltpu
from jax.sharding import PartitionSpec as P

HEAD_DIM = 256
CONV = 4
LAYERS = 2
epsilon = 1e-06
very_negative = -1e30

VM = pl.BlockSpec(memory_space=pltpu.VMEM)
MESH = pl.DeviceIdType.MESH


def greet(axis, devices):
    barrier = pltpu.get_barrier_semaphore()
    for device in devices:
        pl.semaphore_signal(barrier, inc=1, device_id={axis: device}, device_id_type=MESH)
    pl.semaphore_wait(barrier, len(devices))


def rcopy(src, dst, send, recv, axis, device):
    return pltpu.make_async_remote_copy(
        src_ref=src, dst_ref=dst, send_sem=send, recv_sem=recv,
        device_id={axis: device}, device_id_type=MESH,
    )


def scatter_kernel(n, chunks, a_ref, b_ref, aux_ref, oa_ref, ob_ref, oaux_ref,
                   r1a, r1b, s2a, s2b, r2a, r2b, s1s, s1r, s2s, s2r, axs, axr):
    nx = n // 2
    me = lax.axis_index("dp")
    core = me % 2
    x = me // 2
    partner = me + 1 - 2 * core
    greet("dp", [(me + off) % n for off in range(1, n)])
    started = []
    aux_copies = []
    first = {}
    for g in range(nx):
        xo = (x + 1 + g) % nx
        for c in range(chunks):
            pair = []
            for k, (src, dst) in enumerate(((a_ref, r1a), (b_ref, r1b))):
                cp = rcopy(src.at[xo, 1 - core, c], dst.at[g, c],
                           s1s.at[g, c, k], s1r.at[g, c, k], "dp", partner)
                cp.start()
                pair.append(cp)
                started.append(cp)
            first[g, c] = pair
        if g == 0:
            for off in range(1, n):
                to = (me + off) % n
                cp = rcopy(aux_ref.at[to], oaux_ref.at[me], axs.at[off - 1], axr.at[off - 1], "dp", to)
                cp.start()
                aux_copies.append(cp)
                started.append(cp)
            oaux_ref[me] = aux_ref[me]
    second = {}
    for g in range(nx - 1):
        xo = (x + 1 + g) % nx
        for c in range(chunks):
            pair = []
            for k, (src, got, buf, dst) in enumerate(((a_ref, r1a, s2a, r2a), (b_ref, r1b, s2b, r2b))):
                first[g, c][k].wait_recv()
                buf[g, c] = (
                    src[xo, core, c].astype(jnp.float32) + got[g, c].astype(jnp.float32)
                ).astype(jnp.bfloat16)
                cp = rcopy(buf.at[g, c], dst.at[g, c], s2s.at[g, c, k], s2r.at[g, c, k],
                           "dp", 2 * xo + core)
                cp.start()
                pair.append(cp)
                started.append(cp)
            second[g, c] = pair
    for c in range(chunks):
        for k, (src, got, more, out) in enumerate(((a_ref, r1a, r2a, oa_ref), (b_ref, r1b, r2b, ob_ref))):
            first[nx - 1, c][k].wait_recv()
            total = src[x, core, c].astype(jnp.float32) + got[nx - 1, c].astype(jnp.float32)
            for g in range(nx - 1):
                second[g, c][k].wait_recv()
                total = total + more[g, c].astype(jnp.float32)
            out[c] = total
    for cp in aux_copies:
        cp.wait_recv()
    for cp in started:
        cp.wait_send()


def scatter_dp(n, a, b, aux):
    rows, width = a.shape
    nx = n // 2
    own = rows // n
    chunks = 4 if own % 64 == 0 else 1
    piece = own // chunks
    a = a.reshape(nx, 2, chunks, piece, width)
    b = b.reshape(nx, 2, chunks, piece, width)
    far = max(nx - 1, 1)
    bf = jnp.bfloat16
    sem = pltpu.SemaphoreType.DMA
    oa, ob, oaux = pl.pallas_call(
        functools.partial(scatter_kernel, n, chunks),
        out_shape=(
            jax.ShapeDtypeStruct((chunks, piece, width), jnp.float32),
            jax.ShapeDtypeStruct((chunks, piece, width), jnp.float32),
            jax.ShapeDtypeStruct(aux.shape, jnp.float32),
        ),
        in_specs=[VM] * 3,
        out_specs=(VM,) * 3,
        scratch_shapes=[
            pltpu.VMEM((nx, chunks, piece, width), bf),
            pltpu.VMEM((nx, chunks, piece, width), bf),
            pltpu.VMEM((far, chunks, piece, width), bf),
            pltpu.VMEM((far, chunks, piece, width), bf),
            pltpu.VMEM((far, chunks, piece, width), bf),
            pltpu.VMEM((far, chunks, piece, width), bf),
            sem((nx, chunks, 2)), sem((nx, chunks, 2)),
            sem((far, chunks, 2)), sem((far, chunks, 2)),
            sem((n - 1,)), sem((n - 1,)),
        ],
        compiler_params=pltpu.CompilerParams(collective_id=0, has_side_effects=True),
        name="scatter_dp",
    )(a, b, aux)
    return oa.reshape(own, width), ob.reshape(own, width), oaux


def gather_kernel(n, chunks, m_ref, out_ref, xs, xr, ps, pr, fs, fr):
    nx = n // 2
    me = lax.axis_index("dp")
    core = me % 2
    x = me // 2
    partner = me + 1 - 2 * core
    greet("dp", [partner] + [2 * ((x + 1 + g) % nx) + core for g in range(nx - 1)])
    started = []
    across = {}
    near = {}
    for c in range(chunks):
        for g in range(nx - 1):
            to = 2 * ((x + 1 + g) % nx) + core
            cp = rcopy(m_ref.at[c], out_ref.at[x, core, c], xs.at[g, c], xr.at[g, c], "dp", to)
            cp.start()
            across[g, c] = cp
            started.append(cp)
    for c in range(chunks):
        cp = rcopy(m_ref.at[c], out_ref.at[x, core, c], ps.at[c], pr.at[c], "dp", partner)
        cp.start()
        near[c] = cp
        started.append(cp)
    out_ref[x, core] = m_ref[...]
    passed = []
    for c in range(chunks):
        for g in range(nx - 1):
            origin = (x + nx - 1 - g) % nx
            across[g, c].wait_recv()
            cp = rcopy(out_ref.at[origin, core, c], out_ref.at[origin, core, c],
                       fs.at[g, c], fr.at[g, c], "dp", partner)
            cp.start()
            passed.append(cp)
            started.append(cp)
    for c in range(chunks):
        near[c].wait_recv()
    for cp in passed:
        cp.wait_recv()
    for cp in started:
        cp.wait_send()


def gather_dp(n, m):
    own, width = m.shape
    nx = n // 2
    chunks = 4 if own % 64 == 0 else 1
    piece = own // chunks
    far = max(nx - 1, 1)
    sem = pltpu.SemaphoreType.DMA
    out = pl.pallas_call(
        functools.partial(gather_kernel, n, chunks),
        out_shape=jax.ShapeDtypeStruct((nx, 2, chunks, piece, width), m.dtype),
        in_specs=[VM],
        out_specs=VM,
        scratch_shapes=[
            sem((far, chunks)), sem((far, chunks)), sem((chunks,)), sem((chunks,)),
            sem((far, chunks)), sem((far, chunks)),
        ],
        compiler_params=pltpu.CompilerParams(collective_id=1, has_side_effects=True),
        name="gather_dp",
    )(m.reshape(chunks, piece, width))
    return out.reshape(n * own, width)


def reduce_kernel(n, p_ref, x_ref, out_ref, got, mine, s1, r1, s2, r2):
    me = lax.axis_index("tp")
    greet("tp", [(me + off) % n for off in range(1, n)])
    started = []
    first = []
    order = sorted(range(1, n), key=lambda off: -min(off, n - off))
    for off in order:
        to = (me + off) % n
        cp = rcopy(p_ref.at[to], got.at[off - 1], s1.at[off - 1], r1.at[off - 1], "tp", to)
        cp.start()
        started.append(cp)
        first.append((off, cp))
    total = p_ref[me].astype(jnp.float32)
    for off, cp in first:
        cp.wait_recv()
        total = total + got[off - 1].astype(jnp.float32)
    update = total.astype(jnp.bfloat16).astype(jnp.float32)
    mine[...] = (x_ref[me].astype(jnp.float32) + update).astype(jnp.bfloat16)
    second = []
    for off in order:
        to = (me + off) % n
        cp = rcopy(mine, out_ref.at[me], s2.at[off - 1], r2.at[off - 1], "tp", to)
        cp.start()
        started.append(cp)
        second.append(cp)
    out_ref[me] = mine[...]
    for cp in second:
        cp.wait_recv()
    for cp in started:
        cp.wait_send()


def reduce_tp(n, p, x):
    rows, width = p.shape
    share = rows // n
    sem = pltpu.SemaphoreType.DMA
    out = pl.pallas_call(
        functools.partial(reduce_kernel, n),
        out_shape=jax.ShapeDtypeStruct((n, share, width), jnp.bfloat16),
        in_specs=[VM] * 2,
        out_specs=VM,
        scratch_shapes=[
            pltpu.VMEM((n - 1, share, width), jnp.bfloat16),
            pltpu.VMEM((share, width), jnp.bfloat16),
            sem((n - 1,)), sem((n - 1,)), sem((n - 1,)), sem((n - 1,)),
        ],
        compiler_params=pltpu.CompilerParams(collective_id=2, has_side_effects=True),
        name="reduce_tp",
    )(p.reshape(n, share, width), x.reshape(n, share, width))
    return out.reshape(rows, width)


def cell_kernel(per, heads, low, q_ref, k_ref, v_ref, w_ref, s_ref, g_ref, c_ref, *rest):
    num_ref, new_ref = rest[-2:]
    narrow = jnp.bfloat16 if low else jnp.float32
    for i in range(per):
        for h in range(heads):
            q = q_ref[i, h]
            k = k_ref[i, h]
            v = v_ref[i, h]
            scal = s_ref[i, h]
            old = c_ref[0, i, h]
            outer = lax.dot_general(
                (k * scal[:, 1:2]).astype(narrow), v.astype(narrow), (((0,), (0,)), ((), ())),
                preferred_element_type=jnp.float32,
            )
            new_ref[0, i, h] = scal[0:1, 2:3] * old + outer
            carried = jnp.dot(
                q.astype(jnp.bfloat16), old.astype(jnp.bfloat16), preferred_element_type=jnp.float32
            )
            scores = lax.dot_general(
                q.astype(narrow), k.astype(narrow), (((1,), (1,)), ((), ())),
                preferred_element_type=jnp.float32,
            )
            scores = scores * w_ref[i, h]
            inside = jnp.dot(
                scores.astype(narrow), v.astype(narrow), preferred_element_type=jnp.float32
            )
            num = inside + scal[:, 0:1] * carried
            centered = num - jnp.mean(num, axis=-1, keepdims=True)
            spread = jnp.mean(centered * centered, axis=-1, keepdims=True)
            num_ref[i, h] = centered * lax.rsqrt(spread + epsilon) * g_ref[h:h + 1, :]


def memory_cell(layer, q, k, v, weights, scal, gain, memory, previous, per=4, low=True):
    batch, heads, steps, dim = q.shape
    per = per if batch % per == 0 else 1
    row = pl.BlockSpec((per, heads, steps, dim), lambda b: (b, 0, 0, 0))
    small = pl.BlockSpec((per, heads, steps, steps), lambda b: (b, 0, 0, 0))
    three = pl.BlockSpec((per, heads, steps, 3), lambda b: (b, 0, 0, 0))
    mat = pl.BlockSpec((1, per, heads, dim, dim), lambda b: (layer, b, 0, 0, 0))
    args = [q, k, v, weights, scal, gain, memory]
    specs = [row, row, row, small, three, pl.BlockSpec((heads, dim), lambda b: (0, 0)), mat]
    aliases = {}
    if previous is not None:
        args.append(previous)
        specs.append(pl.BlockSpec(memory_space=pl.ANY))
        aliases = {7: 1}
    return pl.pallas_call(
        functools.partial(cell_kernel, per, heads, low),
        grid=(batch // per,),
        out_shape=(
            jax.ShapeDtypeStruct(q.shape, jnp.float32),
            jax.ShapeDtypeStruct(memory.shape, jnp.float32),
        ),
        in_specs=specs,
        out_specs=(row, mat),
        input_output_aliases=aliases,
        compiler_params=pltpu.CompilerParams(dimension_semantics=("arbitrary",)),
        name="memory_cell",
    )(*args)


def per_device(tokens, live_counts, norm_gain, w_branch, w_silu_gate, conv_weight, w_query, w_key,
               w_value, w_input_gate, w_forget_gate, bias_input, bias_forget, out_gain, skip_gain,
               w_out, conv_state, memory, max_state):
    f32 = jnp.float32
    bf = jnp.bfloat16
    ndp = lax.axis_size("dp")
    ntp = lax.axis_size("tp")
    all_batch, steps, features = tokens.shape
    batch = live_counts.shape[0]
    width = w_branch.shape[2]
    heads = w_query.shape[1]
    rows = all_batch * steps
    own = batch * steps
    live_rows = all_batch * steps // 2
    lanes = -(-own // 128) * 128
    model = features * ndp
    flat_tokens = tokens.reshape(rows, features)
    positions = jnp.arange(steps, dtype=jnp.int32)
    live = positions[None, :] < live_counts[:, None]
    causal = positions[:, None] >= positions[None, :]
    picks = live_counts[:, None] + jnp.arange(CONV - 1, dtype=jnp.int32)[None, :]
    pick_hot = picks[:, :, None] == jnp.arange(steps + CONV - 1, dtype=jnp.int32)[None, None, :]
    count_row = jnp.pad(live_counts.astype(f32), (0, lanes - batch))

    dense = flat_tokens
    compact = None
    select = None
    live_all = None
    new_memory = None
    conv_list = []
    max_list = []
    for l in range(LAYERS):
        floats = dense.astype(f32)
        squares = jnp.sum(floats * floats, axis=-1).reshape(ndp, own)
        squares = jnp.pad(squares, ((0, 0), (0, lanes - own)))
        aux = jnp.stack([squares, jnp.broadcast_to(count_row, squares.shape)], axis=1)
        aux = jnp.pad(aux, ((0, 0), (0, 6), (0, 0)))
        scaled = lax.optimization_barrier((floats * norm_gain[l]).astype(bf))
        first = jnp.dot(scaled, w_branch[l], preferred_element_type=f32).astype(bf)
        second = jnp.dot(scaled, w_silu_gate[l], preferred_element_type=f32).astype(bf)
        branch, gate, aux = scatter_dp(ndp, first, second, aux)
        total = jnp.sum(aux[:, 0, :own], axis=0)
        inv = lax.rsqrt(total / model + epsilon)[:, None]
        branch = (branch * inv).astype(bf).reshape(batch, steps, width)
        gate = (gate * inv).astype(bf).astype(f32).reshape(batch, steps, width)
        if select is None:
            counts = aux[:, 1, :batch].astype(jnp.int32).reshape(all_batch)
            ids = jnp.arange(all_batch)
            before = jnp.sum(jnp.where(ids[None, :] < ids[:, None], counts[None, :], 0), axis=1)
            live_all = positions[None, :] < counts[:, None]
            place = jnp.where(live_all, before[:, None] + positions[None, :], -1).reshape(rows)
            select = (jnp.arange(live_rows)[:, None] == place[None, :]).astype(bf)
            select = lax.optimization_barrier(select)
            compact = jnp.dot(select, flat_tokens, preferred_element_type=f32).astype(bf)

        padded = jnp.concatenate([conv_state[l], branch], axis=1).astype(f32)
        conv_sum = padded[:, 0:steps] * conv_weight[l, 0]
        for j in range(1, CONV):
            conv_sum = conv_sum + padded[:, j:j + steps] * conv_weight[l, j]
        convolved = jax.nn.silu(conv_sum).astype(bf)
        new_conv = jnp.stack(
            [jnp.sum(jnp.where(pick_hot[:, i, :, None], padded, 0.0), axis=1) for i in range(CONV - 1)],
            axis=1,
        ).astype(bf)
        conv_list.append(new_conv)
        conv_flat = convolved.reshape(own, width)
        branch_flat = branch.reshape(own, width)

        def project(source, w):
            parts = [
                jnp.dot(source[:, h * HEAD_DIM:(h + 1) * HEAD_DIM], w[h], preferred_element_type=f32)
                for h in range(heads)
            ]
            out = jnp.stack([p.reshape(batch, steps, HEAD_DIM) for p in parts], axis=1)
            return out.astype(bf).astype(f32)

        q = project(conv_flat, w_query[l])
        k = project(conv_flat, w_key[l])
        v = project(branch_flat, w_value[l])

        def gate_dot(w, bias):
            w = w.astype(f32).reshape(heads, 3, 1, HEAD_DIM)
            return jnp.sum(q * w[:, 0] + k * w[:, 1] + v * w[:, 2], axis=-1) + bias[:, None]

        live_h = live[:, None, :]
        ig = jnp.where(live_h, gate_dot(w_input_gate[l], bias_input[l]), very_negative)
        fg = jnp.where(live_h, jax.nn.log_sigmoid(gate_dot(w_forget_gate[l], bias_forget[l])), 0.0)
        cum = jnp.sum(jnp.where(causal, fg[..., None, :], 0.0), axis=-1)
        logw = cum[..., :, None] - cum[..., None, :] + ig[..., None, :]
        logw = jnp.where(causal, logw, very_negative)
        carried = cum + max_state[l][..., None]
        stab = jnp.maximum(jnp.max(logw, axis=-1), carried)
        weights = jnp.exp(logw - stab[..., None])
        new_max = stab[..., -1]
        decay = jnp.exp(cum[..., -1] + max_state[l] - new_max)
        upd = jnp.exp(cum[..., -1:] - cum + ig - new_max[..., None])
        scal = jnp.stack(
            [jnp.exp(carried - stab), upd, jnp.broadcast_to(decay[..., None], upd.shape)], axis=-1
        )
        max_list.append(new_max)
        normalized, new_memory = memory_cell(
            l, q, k * HEAD_DIM ** (-0.5), v, weights, scal, out_gain[l], memory, new_memory
        )
        readout = jnp.transpose(normalized, (0, 2, 1, 3)).reshape(batch, steps, width)
        mixed = (readout + skip_gain[l] * convolved.astype(f32)) * jax.nn.silu(gate)
        mixed = jnp.where(live[:, :, None], mixed, 0.0).astype(bf).reshape(own, width)
        everyone = gather_dp(ndp, mixed)
        packed = jnp.dot(select, everyone, preferred_element_type=f32).astype(bf)
        part = jnp.dot(packed, w_out[l], preferred_element_type=f32).astype(bf)
        compact = reduce_tp(ntp, part, compact)
        dense = lax.dot_general(
            select, compact, (((0,), (0,)), ((), ())), preferred_element_type=f32
        ).astype(bf)
    result = jnp.where(live_all[:, :, None], dense.reshape(tokens.shape), tokens)
    return (result, jnp.stack(conv_list), new_memory, jnp.stack(max_list))


def solution(mesh):
    in_specs = (
        P("grp", None, "dp"),
        P(("grp", "dp")),
        P(None, "dp"),
        P(None, "dp", "tp"),
        P(None, "dp", "tp"),
        P(None, None, "tp"),
        P(None, "tp", None, None),
        P(None, "tp", None, None),
        P(None, "tp", None, None),
        P(None, "tp", None),
        P(None, "tp", None),
        P(None, "tp"),
        P(None, "tp"),
        P(None, "tp", None),
        P(None, "tp"),
        P(None, "tp", "dp"),
        P(None, ("grp", "dp"), None, "tp"),
        P(None, ("grp", "dp"), "tp", None, None),
        P(None, ("grp", "dp"), "tp"),
    )
    out_specs = (
        P("grp", None, "dp"),
        P(None, ("grp", "dp"), None, "tp"),
        P(None, ("grp", "dp"), "tp", None, None),
        P(None, ("grp", "dp"), "tp"),
    )
    return jax.shard_map(
        per_device, mesh=mesh, in_specs=in_specs, out_specs=out_specs, check_vma=False
    )
```
